32 devices in a mesh: sp: 16 (over z, y, x), tp: 2 (over core).
Axes of the slice: x: 2, y: 2, z: 4, core: 2. Of those that a mesh axis runs over, the one named last changes fastest.
Arguments:
- resid: bfloat16 [4096, 2048], P(('sp', 'tp')), may hold values from -6 to 6
- value_in: bfloat16 [4096, 1536], P('sp', 'tp'), may hold values from -6 to 6
- gate_in: bfloat16 [4096, 1536], P('sp', 'tp'), may hold values from -8 to 8
- conv_weight: float32 [31, 1536], P(None, 'tp'), may hold values from -2.5 to 2.5
- norm_gain: float32 [1536], P('tp'), may hold values from 0.1 to 1.9
- out_weight: bfloat16 [1536, 2048], replicated, may hold values from -0.15625 to 0.15625
- ffn_gain: float32 [2048], replicated, may hold values from 0.1 to 1.9
- expert_ids: int32 [4096, 2], P(('sp', 'tp')), may hold values from 0 to 31, all different within a row; in each aligned block of 128 rows (0 to 127, 128 to 255, ...) at most 16 rows name the same one
- expert_mix: float32 [4096, 2], P(('sp', 'tp')), may hold values from 0.1 to 1
- w_gate: bfloat16 [32, 2048, 1024], P(('sp', 'tp')), may hold values from -0.125 to 0.125
- w_up: bfloat16 [32, 2048, 1024], P(('sp', 'tp')), may hold values from -0.125 to 0.125
- w_down: bfloat16 [32, 1024, 2048], P(('sp', 'tp')), may hold values from -0.1875 to 0.1875
Outputs:
- layer_out: bfloat16 [4096, 2048], P(('sp', 'tp'))
The draws below stay inside these ranges and needn't reach their ends.
Inputs may be any that keep to these rules, and one draw needn't show every extreme that they name: `expert_ids`: each row names 2 different experts; within each aligned block of 128 rows no expert is named by more than 16 rows, a bound that some block reaches.
All inputs are finite; a program needn't handle non-finite values.
Results may differ from the reference program's by a relative error of at most 0.012.
Values may be sent and summed in bfloat16 or wider, within the bound.
A program may use at most 128 MiB of HBM per device.

```python
import math
import jax
import jax.numpy as jnp
import numpy as np
from jax import lax

D = 2048
MIX = 1536
FF = 1024
CONV = 31
TOPK = 2
TOKENS = 4096
ROWS = 128
EXPERTS = 32
CAP = 16


def draw_conv_weight(key, part):
    first = jax.random.fold_in(key, 0)
    place = jnp.arange(MIX, dtype=jnp.float32) / max(MIX - 1, 1)
    scale = jnp.exp(jnp.log(4.0) * place)
    taps = jax.random.normal(first, (CONV, MIX), jnp.float32) * CONV ** (-0.5) * scale
    return jnp.clip(taps, -2.5, 2.5)


def steps_of(rng, extent, cuts, least, top_value):
    level = 1.0
    for dim, shards_of in cuts:
        steps = jax.random.uniform(jax.random.fold_in(jax.random.fold_in(rng, 6), dim), (shards_of,), jnp.float32, least / len(cuts), top_value / len(cuts))
        level = level * jnp.repeat(jnp.exp(steps), extent[dim] // shards_of).reshape((-1,) + (1,) * (len(extent) - 1 - dim))
    return level


def shared_out(stream_key, own, number, rows, number_of, top, bound, slope):
    ranking = jax.random.permutation(stream_key, number_of)
    packed, ordinary = portions_of(number_of, rows * top, bound, slope, True), portions_of(number_of, rows * top, bound, slope, False)
    places = jnp.arange(number_of)

    def named(tallies, turn):
        used = int((tallies > 0).sum())
        fixed = max(1, used // 4)
        passed = fixed + (places - fixed + turn * (used - fixed)) % max(1, number_of - fixed)
        return jnp.zeros((number_of,), jnp.int32).at[ranking[jnp.where(places < fixed, places, passed)]].set(jnp.asarray(tallies, jnp.int32))

    tallies = jnp.where(number % 4 == 0, named(packed, number // 4), named(ordinary, number - number // 4 - 1))
    mixed = jax.random.permutation(jax.random.fold_in(own, 3), number_of)
    source_of, sink = mixed[0:number_of // 2 * 2:2], mixed[1:number_of // 2 * 2:2]
    room = jnp.minimum(tallies[source_of] - 1, bound - tallies[sink]) // 2
    room = jnp.where((source_of == ranking[0]) | (sink == ranking[0]) | (tallies[sink] == 0), 0, jnp.maximum(room, 0))
    passed = jax.random.randint(jax.random.fold_in(own, 4), (number_of // 2,), 0, 1 << 20) % (room + 1)
    tallies = tallies.at[source_of].add(-passed).at[sink].add(passed)
    members = jnp.searchsorted(jnp.cumsum(tallies), jnp.arange(rows * top), side="right").astype(jnp.int32)
    listing = members.reshape(top, rows).T
    listing = listing[jax.random.permutation(jax.random.fold_in(own, 1), rows)]
    turn = jax.random.randint(jax.random.fold_in(own, 2), (rows, 1), 0, top)
    return jnp.take_along_axis(listing, (jnp.arange(top)[None, :] + turn) % top, axis=1)


def portions_of(amount, total, bound, lean, full):
    weights = [(1 << 20) // math.isqrt(grade ** lean) + 1 for grade in range(1, amount + 1)]
    largest = bound if full else min(bound, max(-(-total // amount), total * weights[0] // sum(weights)))
    least = 1 if total - largest >= amount - 1 else 0
    counts, surplus = [largest] + [least] * (amount - 1), total - largest - least * (amount - 1)
    while surplus > 0:
        candidates = [i for i in range(1, amount) if counts[i] < largest] or [i for i in range(1, amount) if counts[i] < bound]
        pool, left = sum([weights[i] for i in candidates]), surplus
        for i in candidates:
            more = min(bound - counts[i], max(1, left * weights[i] // pool), surplus)
            counts[i] = counts[i] + more
            surplus = surplus - more
    return np.array(counts)


def centred(own_key, dims, spread, limit, cuts=(), held_as=jnp.bfloat16):
    gain = steps_of(own_key, dims, cuts, -0.22, 0.18) if cuts else 1.0
    drawn = jax.random.normal(own_key, dims, jnp.float32) * spread * gain
    return jnp.minimum(jnp.maximum(drawn, -limit), limit).astype(held_as)


def setup_inputs(seed: int = 0) -> dict:
    streams_of = jax.random.split(jax.random.key(seed), 13)
    resid = centred(streams_of[0], (TOKENS, D), 1.0, 6.0, ((0, 32),))
    value_in = centred(streams_of[1], (TOKENS, MIX), 1.0, 6.0, ((0, 16), (1, 2)))
    gate_in = centred(streams_of[2], (TOKENS, MIX), 1.5, 8.0, ((0, 16), (1, 2)))
    conv_weight = draw_conv_weight(jax.random.fold_in(streams_of[12], 71), 0)
    norm_gain = jnp.clip(1.0 + 0.18 * jax.random.normal(streams_of[4], (MIX,), jnp.float32), 0.1, 1.9)
    out_weight = centred(streams_of[5], (MIX, D), MIX ** -0.5, 0.15625)
    ffn_gain = jnp.clip(1.0 + 0.18 * jax.random.normal(streams_of[6], (D,), jnp.float32), 0.1, 1.9)
    expert_ids_keys = jax.random.split(jax.random.fold_in(streams_of[7], 1), TOKENS // ROWS)
    expert_ids_turns = jax.random.permutation(jax.random.fold_in(streams_of[7], 3), TOKENS // ROWS)
    expert_ids = jax.vmap(lambda own, number: shared_out(jax.random.fold_in(streams_of[7], 2), own, number, ROWS, EXPERTS, TOPK, CAP, 2))(expert_ids_keys, expert_ids_turns).reshape((TOKENS, TOPK))
    expert_mix = jnp.clip(0.1 + 0.9 * jax.random.uniform(streams_of[8], (TOKENS, TOPK), jnp.float32) ** steps_of(streams_of[8], (TOKENS, TOPK), ((0, 32),), -0.2, 0.2), 0.1, 1.0)
    w_gate = centred(streams_of[9], (EXPERTS, D, FF), D ** -0.5, 0.125, ((0, 32),))
    w_up = centred(streams_of[10], (EXPERTS, D, FF), D ** -0.5, 0.125, ((0, 32),))
    w_down = centred(streams_of[11], (EXPERTS, FF, D), FF ** -0.5, 0.1875, ((0, 32),))
    return {"resid": resid, "value_in": value_in, "gate_in": gate_in, "conv_weight": conv_weight, "norm_gain": norm_gain, "out_weight": out_weight, "ffn_gain": ffn_gain, "expert_ids": expert_ids, "expert_mix": expert_mix, "w_gate": w_gate, "w_up": w_up, "w_down": w_down}


def reference(resid, value_in, gate_in, conv_weight, norm_gain, out_weight, ffn_gain, expert_ids, expert_mix, w_gate, w_up, w_down):
    glu = (value_in.astype(jnp.float32) * jax.nn.sigmoid(gate_in.astype(jnp.float32))).astype(jnp.bfloat16)
    reach = CONV // 2
    padded = jnp.pad(glu.astype(jnp.float32), ((reach, reach), (0, 0)))
    conv = jnp.zeros((TOKENS, MIX), jnp.float32)
    for tap in range(CONV):
        conv = conv + padded[tap:tap + TOKENS] * conv_weight[tap]
    mean = lax.optimization_barrier(jnp.mean(conv, axis=1, keepdims=True))
    msq = lax.optimization_barrier(jnp.mean(conv * conv, axis=1, keepdims=True))
    var = msq - mean * mean
    mixed = jax.nn.silu((conv - mean) * lax.rsqrt(var + 1e-05) * norm_gain).astype(jnp.bfloat16)
    proj = jnp.dot(mixed, out_weight, preferred_element_type=jnp.float32)
    stream = (resid.astype(jnp.float32) + proj).astype(jnp.bfloat16)
    wide = stream.astype(jnp.float32)
    normed = (wide * lax.rsqrt(lax.optimization_barrier(jnp.mean(wide * wide, axis=1, keepdims=True)) + 1e-06) * ffn_gain).astype(jnp.bfloat16)
    blocks = TOKENS // ROWS
    chosen = expert_ids.reshape(blocks, ROWS * TOPK)
    onehot = (chosen[:, :, None] == jnp.arange(EXPERTS, dtype=jnp.int32)[None, None, :]).astype(jnp.int32)
    rank = lax.optimization_barrier(jnp.sum(jnp.cumsum(onehot, axis=1) * onehot, axis=2)) - 1
    slot = jnp.arange(blocks, dtype=jnp.int32)[:, None] * CAP + rank
    token = jnp.arange(blocks, dtype=jnp.int32)[:, None] * ROWS + jnp.arange(ROWS * TOPK, dtype=jnp.int32)[None, :] // TOPK
    table = jnp.full((EXPERTS, blocks * CAP), TOKENS, jnp.int32)
    table = table.at[chosen.reshape(-1), slot.reshape(-1)].set(token.reshape(-1).astype(jnp.int32))
    source = jnp.concatenate([normed, jnp.zeros((1, D), jnp.bfloat16)], axis=0)

    def run(args):
        index, gate_w, up_w, down_w = args
        rows = jnp.take(source, index, axis=0)
        gate = jnp.dot(rows, gate_w, preferred_element_type=jnp.float32)
        up = jnp.dot(rows, up_w, preferred_element_type=jnp.float32)
        hidden = (jax.nn.silu(gate) * up).astype(jnp.bfloat16)
        return jnp.dot(hidden, down_w, preferred_element_type=jnp.float32).astype(jnp.bfloat16)
    results = lax.map(run, (table, w_gate, w_up, w_down))
    picked = results[chosen.reshape(-1), slot.reshape(-1)].astype(jnp.float32).reshape(TOKENS, TOPK, D)
    total = stream.astype(jnp.float32) + lax.optimization_barrier(jnp.sum(picked * expert_mix[:, :, None], axis=1))
    return total.astype(jnp.bfloat16)
```

```python
import functools
import jax
import jax.numpy as jnp
from jax import lax
from jax.experimental import pallas as pl
from jax.experimental.pallas import tpu as pltpu
from jax.sharding import PartitionSpec as P

MESH = pl.DeviceIdType.MESH
BF = jnp.bfloat16
F32 = jnp.float32


PLANES = 4


def layer_kernel(
    sp_count, tp_count, cap, chunks,
    resid, value_in, gate_in, taps_w, gain, ffn_gain, ids, mix, ow_h, wg_h, wu_h, wd_h, out,
    wg, wu, wd, tok, infos, pack, rx, hid, gates, ups, ys, yr, part, sums, back, acc,
    hots, mixes, ow, gp, wide_in, cs, cf, gf,
    w_sem, i_send, i_recv, t_send, t_recv, d_send, d_recv, r_send, r_recv, b_send, b_recv,
    h_sem, c_sem, g_sem,
):
    plane = sp_count // PLANES
    n_dev = plane * tp_count
    rows, width = resid.shape
    dc = width // chunks
    slots = n_dev * cap
    me_sp = lax.axis_index("sp")
    me_tp = lax.axis_index("tp")
    local = lax.rem(me_sp, plane)
    base = me_sp - local
    mine = local * tp_count + me_tp
    level = me_sp // plane
    low_half = level < PLANES // 2
    step_in = jnp.where(low_half, plane, -plane)
    is_end = (level == 0) | (level == PLANES - 1)
    is_mid = jnp.logical_not(is_end)
    inner = (me_sp + step_in, me_tp)
    outer = (jnp.where(is_mid, me_sp - step_in, me_sp), me_tp)

    def column(i):
        return (lax.rem(me_sp + i * plane, sp_count), me_tp)

    def peer(i):
        n = lax.rem(mine + i, n_dev)
        return n, (base + n // tp_count, lax.rem(n, tp_count))

    weights = [
        pltpu.make_async_copy(h, v, w_sem.at[k])
        for k, (h, v) in enumerate(((ow_h, ow), (wg_h, wg), (wu_h, wu), (wd_h, wd)))
    ]
    for w in weights:
        w.start()

    barrier = pltpu.get_barrier_semaphore()

    @pl.loop(1, n_dev)
    def _(i):
        pl.semaphore_signal(barrier, inc=1, device_id=peer(i)[1], device_id_type=MESH)

    @pl.loop(1, PLANES)
    def _(i):
        pl.semaphore_signal(barrier, inc=1, device_id=column(i), device_id_type=MESH)

    last = sp_count - 1
    has_low, has_high = me_sp > 0, me_sp < last
    lower = (jnp.maximum(me_sp - 1, 0), me_tp)
    upper = (jnp.minimum(me_sp + 1, last), me_tp)
    twin = (me_sp, 1 - me_tp)

    @pl.when(has_low)
    def _():
        pl.semaphore_signal(barrier, inc=1, device_id=lower, device_id_type=MESH)

    @pl.when(has_high)
    def _():
        pl.semaphore_signal(barrier, inc=1, device_id=upper, device_id_type=MESH)

    length, local_width = value_in.shape
    taps = taps_w.shape[0]
    reach = taps // 2
    halo = (reach + 15) // 16 * 16
    half = rows // 2
    span = half + 2 * halo
    gated = (value_in[...].astype(F32) * jax.nn.sigmoid(gate_in[...].astype(F32))).astype(BF)
    gp[halo : halo + length, :] = gated
    wide_in[halo : halo + length, :] = gated.astype(F32)

    @pl.when(jnp.logical_not(has_low))
    def _():
        gp[0:halo, :] = jnp.zeros((halo, local_width), BF)

    @pl.when(jnp.logical_not(has_high))
    def _():
        gp[halo + length :, :] = jnp.zeros((halo, local_width), BF)

    def begins(h, core):
        return pl.multiple_of(half + half * core if h == 0 else (length - half) * core, half)

    def inside(h, core):
        return pl.ds(pl.multiple_of(half * (1 - core) if h == 0 else half * core, half), half)

    def convolve(h, core, put):
        first = begins(h, core)

        @pl.loop(0, local_width // 128)
        def _(b):
            cols = pl.ds(pl.multiple_of(b * 128, 128), 128)
            x = wide_in[pl.ds(first, span), cols]
            total = jnp.zeros((half, 128), F32)
            for r in range(8):
                offsets = [j for j in range(taps) if (j + halo - reach) % 8 == r]
                if not offsets:
                    continue
                shifted = x if r == 0 else pltpu.roll(x, span - r, 0)
                for j in offsets:
                    at = j + halo - reach - r
                    total = total + shifted[at : at + half] * taps_w[j : j + 1, cols]
            put(cols, total)

    def both(h):
        def put_out(cols, total):
            cs[h, :, cols] = total

        def put_own(cols, total):
            cf[0, inside(h, me_tp), cols] = total

        return put_out, put_own

    convolve(0, 1 - me_tp, both(0)[0])
    convolve(0, me_tp, both(0)[1])

    pl.semaphore_wait(
        barrier,
        n_dev - 1 + PLANES - 1 + has_low.astype(jnp.int32) + has_high.astype(jnp.int32),
    )

    def remote(src, dst, send, recv, where):
        return pltpu.make_async_remote_copy(
            src_ref=src, dst_ref=dst, send_sem=send, recv_sem=recv,
            device_id=where, device_id_type=MESH,
        )

    to_low = remote(
        gp.at[halo : 2 * halo], gp.at[halo + length : 2 * halo + length], h_sem.at[0], h_sem.at[1], lower
    )
    to_high = remote(gp.at[length : length + halo], gp.at[0:halo], h_sem.at[2], h_sem.at[3], upper)

    @pl.when(has_low)
    def _():
        to_low.start()

    @pl.when(has_high)
    def _():
        to_high.start()

    def conv_copy(h):
        there = inside(h, 1 - me_tp)
        return remote(cs.at[h], cf.at[1, there], c_sem.at[0, h], c_sem.at[1, h], twin)

    conv_copy(0).start()
    gain_copy = remote(gain, gf, g_sem.at[0], g_sem.at[1], twin)
    gain_copy.start()

    experts_all = sp_count * tp_count
    expert = lax.broadcasted_iota(jnp.int32, (experts_all, rows), 0).astype(F32)
    named = ids[...].astype(F32)
    hot = [jnp.where(expert == named[k : k + 1, :], 1.0, 0.0) for k in range(2)]
    earlier = lax.broadcasted_iota(jnp.int32, (rows, rows), 0)
    later = lax.broadcasted_iota(jnp.int32, (rows, rows), 1)
    before = jnp.where(earlier < later, 1.0, 0.0).astype(BF)
    rank = jnp.dot((hot[0] + hot[1]).astype(BF), before, preferred_element_type=F32)
    infos[0, 2:4, :] = mix[...]
    infos[0, 4:, :] = jnp.zeros((4, rows), F32)
    for k in range(2):
        infos[0, k : k + 1, :] = named[k : k + 1, :] * cap + jnp.sum(
            hot[k] * rank, axis=0, keepdims=True
        )

    def place(there):
        at_end = (there == 0) | (there == PLANES - 1)
        gap = jnp.abs(there - level)
        return jnp.where(at_end, gap, jnp.where(is_end, jnp.where(gap == 1, 1, 3), 2))

    info_copies = []
    for i in range(1, PLANES):
        there = lax.rem(level + i, PLANES)
        info_copies.append(
            remote(infos.at[0], infos.at[place(there)], i_send.at[i], i_recv.at[place(there)], column(i))
        )
    for copy in info_copies:
        copy.start()

    channels = local_width * tp_count
    whose = (me_tp, 1 - me_tp)
    step = 512

    def silu(v):
        return v * jax.nn.sigmoid(v)

    def hop(q, src, k, c, where):
        return remote(tok.at[src, c], tok.at[k, c], t_send.at[q, c], t_recv.at[k, c], where)

    def hop_part(q, k, c, where, at):
        return remote(tok.at[0, c, at], tok.at[k, c, at], t_send.at[q, c], t_recv.at[k, c], where)

    def tokens(h):
        here = inside(h, me_tp)
        remote(cs.at[h], cf.at[1, here], c_sem.at[0, h], c_sem.at[1, h], twin).wait_recv()
        conv = [cf[i, here, :] for i in range(2)]
        mean = sum(jnp.sum(v, axis=1, keepdims=True) for v in conv) / channels
        msq = sum(jnp.sum(v * v, axis=1, keepdims=True) for v in conv) / channels
        scale = lax.rsqrt(msq - mean * mean + 1e-05)
        mixed = [
            silu((v - mean) * scale * g[...].reshape(1, local_width)).astype(BF)
            for v, g in zip(conv, (gain, gf))
        ]
        square = jnp.zeros((half, 1), F32)
        for c in range(width // step):
            cols = slice(c * step, (c + 1) * step)
            proj = jnp.zeros((half, step), F32)
            for m, w in zip(mixed, whose):
                at = pl.ds(pl.multiple_of(w * local_width, local_width), local_width)
                proj = proj + jnp.dot(m, ow[at, cols], preferred_element_type=F32)
            wide = (resid[here, cols].astype(F32) + proj).astype(BF).astype(F32)
            acc[here, cols] = wide
            square = square + jnp.sum(wide * wide, axis=1, keepdims=True)
        rms = lax.rsqrt(square / width + 1e-06)
        for c in range(chunks):
            at = slice(c * dc, (c + 1) * dc)
            tok[0, c, here, :] = (acc[here, at] * rms * ffn_gain[:, at]).astype(BF)

            @pl.when(is_mid)
            def _():
                hop_part(0, 2, c, inner, here).start()
                hop_part(1, 1, c, outer, here).start()

            @pl.when(is_end)
            def _():
                hop_part(0, 1, c, inner, here).start()

    weights[0].wait()
    gain_copy.wait_recv()
    tokens(0)

    @pl.when(has_low)
    def _():
        to_high.wait_recv()

    @pl.when(has_high)
    def _():
        to_low.wait_recv()

    wide_in[0:halo, :] = gp[0:halo, :].astype(F32)
    wide_in[halo + length :, :] = gp[halo + length :, :].astype(F32)
    convolve(1, 1 - me_tp, both(1)[0])
    conv_copy(1).start()
    convolve(1, me_tp, both(1)[1])
    tokens(1)

    def slot_match(ref):
        ids = lax.broadcasted_iota(jnp.int32, (slots, rows), 0) + base * (tp_count * cap)
        ids = ids.astype(F32)
        return ids == ref[0:1, :], ids == ref[1:2, :]

    def tables(k):
        a, b = slot_match(infos.at[k])
        hots[k] = jnp.where(a | b, 1.0, 0.0).astype(BF)
        full = jnp.where(a, infos[k, 2:3, :], 0.0) + jnp.where(b, infos[k, 3:4, :], 0.0)
        full = jnp.transpose(full)
        high = full.astype(BF)
        mixes[k, :, :slots] = high
        mixes[k, :, slots:] = (full - high.astype(F32)).astype(BF)

    few = n_dev <= 8
    peers = [peer(i) for i in range(1, n_dev)] if few else []

    def exchange(src, dst, send, recv, k, c):
        def start(n, where):
            remote(src.at[k, c, n], dst.at[k, c, mine], send.at[k, c], recv.at[k, c], where).start()

        if few:
            for n, where in peers:
                start(n, where)
        else:

            @pl.loop(1, n_dev)
            def _(i):
                start(*peer(i))

        dst[k, c, mine] = src[k, c, mine]

    def all_in(dst, recv, k, c):
        share = dst.at[k, c, pl.ds(0, n_dev - 1)]
        pltpu.make_async_copy(share, share, recv.at[k, c]).wait()

    def all_out(src, send, k, c):
        share = src.at[k, c, pl.ds(0, n_dev - 1)]
        pltpu.make_async_copy(share, share, send.at[k, c]).wait()

    def dispatch(k, c):
        picked = jnp.dot(hots[k], tok[k, c], preferred_element_type=F32)
        pack[k, c] = picked.astype(BF).reshape(n_dev, cap, dc)
        exchange(pack, rx, d_send, d_recv, k, c)

    def arrived(k, c):
        hop(0, k, k, c, inner).wait_recv()

    ff = wg.shape[1]
    tile = min(256, ff)
    pairs = chunks // 2

    def hidden(*ks):
        for k in ks:
            for c in range(chunks):
                all_in(rx, d_recv, k, c)
        n = len(ks) * slots

        @pl.loop(0, ff // tile)
        def _(f):
            cols = pl.ds(pl.multiple_of(f * tile, tile), tile)
            gate = jnp.zeros((n, tile), F32)
            up = jnp.zeros((n, tile), F32)
            for c in range(chunks):
                x = [rx[k, c].reshape(slots, dc) for k in ks]
                x = x[0] if len(ks) == 1 else jnp.concatenate(x, axis=0)
                at = slice(c * dc, (c + 1) * dc)
                gate = gate + jnp.dot(x, wg[at, cols], preferred_element_type=F32)
                up = up + jnp.dot(x, wu[at, cols], preferred_element_type=F32)
            made = (gate * jax.nn.sigmoid(gate) * up).astype(BF)
            for i, k in enumerate(ks):
                hid[k, :, cols] = made[i * slots : (i + 1) * slots]

    def hidden_part(k, j):
        for c in (2 * j, 2 * j + 1):
            all_in(rx, d_recv, k, c)

        @pl.loop(0, ff // tile)
        def _(f):
            cols = pl.ds(pl.multiple_of(f * tile, tile), tile)
            gate = up = None
            for c in (2 * j, 2 * j + 1):
                x = rx[k, c].reshape(slots, dc)
                at = slice(c * dc, (c + 1) * dc)
                g = jnp.dot(x, wg[at, cols], preferred_element_type=F32)
                u = jnp.dot(x, wu[at, cols], preferred_element_type=F32)
                gate, up = (g, u) if gate is None else (gate + g, up + u)
            if j > 0:
                gate, up = gate + gates[:, cols], up + ups[:, cols]
            if j < pairs - 1:
                gates[:, cols] = gate
                ups[:, cols] = up
            else:
                hid[k, :, cols] = (gate * jax.nn.sigmoid(gate) * up).astype(BF)

    def answer(k, c):
        exchange(ys, yr, r_send, r_recv, k, c)

    def down(ks, first, last, send=()):
        for c in range(first, last):
            x = [hid[k] for k in ks]
            x = x[0] if len(ks) == 1 else jnp.concatenate(x, axis=0)
            y = jnp.dot(x, wd[:, c * dc : (c + 1) * dc], preferred_element_type=F32).astype(BF)
            for i, k in enumerate(ks):
                ys[k, c] = y[i * slots : (i + 1) * slots].reshape(n_dev, cap, dc)
                if k in send:
                    answer(k, c)

    def combine(k, c):
        all_in(yr, r_recv, k, c)
        y = yr[k, c].reshape(slots, dc)
        return jnp.dot(mixes[k], jnp.concatenate([y, y], axis=0), preferred_element_type=F32)

    def homeward(q, slot, c, where):
        return remote(sums.at[q, c], back.at[slot, c], b_send.at[q, c], b_recv.at[slot, c], where)

    def returned(slot, c):
        homeward(0, slot, c, inner).wait_recv()
        return back[slot, c].astype(F32)

    def send_home(q, slot, c, where, value):
        sums[q, c] = value.astype(BF)
        homeward(q, slot, c, where).start()

    def add(c, value):
        acc[:, c * dc : (c + 1) * dc] += value

    tables(0)
    for c in range(chunks):
        dispatch(0, c)
    for k in range(1, PLANES):
        remote(infos.at[0], infos.at[k], i_send.at[k], i_recv.at[k], inner).wait_recv()
        tables(k)

    def take(k, *cs):
        for c in cs:
            arrived(k, c)
            dispatch(k, c)

    for w in weights[1:]:
        w.wait()
    every = range(chunks)

    @pl.when(is_end)
    def _():
        def own(*cs):
            for c in cs:
                add(c, combine(0, c))

        def home(k, *cs):
            for c in cs:
                send_home(k - 1, k - 1, c, inner, combine(k, c))

        take(1, 0, 1, 2, 3)
        hidden(0)
        down((0,), 0, 2)
        take(1, 4, 5)
        down((0,), 2, 8)
        take(1, 6, 7)
        take(2, 0, 1)
        hidden(1)
        take(2, 2)
        down((1,), 0, 3, send=(1,))
        take(2, 3)
        down((1,), 3, 8, send=(1,))
        take(2, 4, 5)
        home(1, 0, 1)
        take(2, 6)
        home(1, 2)
        take(2, 7)
        home(1, 3, 4)
        take(3, 0)
        home(1, 5, 6)
        take(3, 1)
        home(1, 7)
        take(3, 2, 3)
        hidden(2)
        down((2,), 0, 1, send=(2,))
        take(3, 4)
        hidden_part(3, 0)
        down((2,), 1, 2, send=(2,))
        hidden_part(3, 1)
        take(3, 5)
        down((2,), 2, 5, send=(2,))
        take(3, 6)
        down((2,), 5, 8, send=(2,))
        home(2, 0)
        take(3, 7)
        home(2, 1, 2)
        hidden_part(3, 2)
        home(2, 3, 4, 5, 6, 7)
        hidden_part(3, 3)
        down((3,), 0, 8, send=(3,))
        for c in every:
            answer(0, c)
        home(3, *every)
        own(*every)
        for c in every:
            at = slice(c * dc, (c + 1) * dc)
            out[:, at] = (acc[:, at] + returned(0, c)).astype(BF)
        for c in range(chunks):
            hop(0, 0, 1, c, inner).wait_send()

    @pl.when(is_mid)
    def _():
        def near(*cs):
            for c in cs:
                arrived(1, c)
                hop(2, 1, 3, c, inner).start()
                dispatch(1, c)
                arrived(2, c)
                hop(3, 2, 2, c, outer).start()
                dispatch(2, c)

        def far(*cs):
            for c in cs:
                arrived(3, c)
                hop(4, 3, 3, c, outer).start()
                dispatch(3, c)

        def keep(k, *cs):
            for c in cs:
                part[k - 1, c] = combine(k, c)

        def pass_on(q, k, slot, got, where, c):
            send_home(q, slot, c, where, part[k - 1, c] + returned(got, c))

        def finish(*cs):
            for c in cs:
                at = slice(c * dc, (c + 1) * dc)
                value = combine(0, c) + returned(0, c) + returned(3, c)
                out[:, at] = (acc[:, at] + value).astype(BF)

        def middle(c):
            pass_on(0, 2, 3, 1, inner, c)

        def onward(c):
            pass_on(1, 3, 4, 2, inner, c)

        near(0, 1, 2, 3)
        hidden(0)
        down((0,), 0, 2)
        near(4, 5)
        down((0,), 2, 8)
        near(6, 7)
        far(0, 1, 2, 3)
        hidden(1, 2)
        down((1, 2), 0, 1, send=(1,))
        far(4)
        down((1, 2), 1, 3, send=(1,))
        far(5)
        down((1, 2), 3, 5, send=(1,))
        far(6)
        down((1, 2), 5, 7, send=(1,))
        keep(1, 0)
        far(7)
        down((1, 2), 7, 8, send=(1,))
        for c in every:
            answer(2, c)
        keep(1, 1, 2, 3, 4, 5, 6)
        hidden(3)
        keep(1, 7)
        keep(2, 0)
        down((3,), 0, 2, send=(3,))
        keep(2, 1)
        down((3,), 2, 5, send=(3,))
        keep(2, 2)
        down((3,), 5, 8, send=(3,))
        for c in every:
            answer(0, c)
        keep(2, 3, 4, 5, 6)
        middle(0)
        keep(2, 7)
        keep(3, 0)
        middle(1)
        keep(3, 1, 2)
        middle(2)
        keep(3, 3, 4)
        middle(3)
        keep(3, 5, 6)
        middle(4)
        keep(3, 7)
        finish(0)
        middle(5)
        finish(1, 2)
        middle(6)
        finish(3, 4)
        middle(7)
        finish(5)
        onward(0)
        finish(6)
        onward(1)
        finish(7)
        for c in range(2, chunks + 2):
            if c < chunks:
                pass_on(1, 3, 4, 2, inner, c)
            pass_on(2, 1, 0, 4, outer, c - 2)
        for c in range(chunks):
            hop(0, 0, 2, c, inner).wait_send()
            hop(1, 0, 1, c, outer).wait_send()
            hop(2, 1, 3, c, inner).wait_send()
            hop(3, 2, 2, c, outer).wait_send()
            hop(4, 3, 3, c, outer).wait_send()

    for copy in info_copies:
        copy.wait_send()
    gain_copy.wait_send()
    conv_copy(0).wait_send()
    conv_copy(1).wait_send()

    @pl.when(has_low)
    def _():
        to_low.wait_send()

    @pl.when(has_high)
    def _():
        to_high.wait_send()

    for c in range(chunks):
        for q in range(3):
            homeward(q, q, c, inner).wait_send()
        for k in range(PLANES):
            all_out(pack, d_send, k, c)
            all_out(ys, r_send, k, c)


def layer_call(resid, value_in, gate_in, taps_w, gain, ffn_gain, ids, mix, ow, w_gate, w_up, w_down, cap):
    sp_count, tp_count = lax.axis_size("sp"), lax.axis_size("tp")
    chunks = 8
    rows, width = resid.shape
    length, local_width = value_in.shape
    halo = (taps_w.shape[0] // 2 + 15) // 16 * 16
    n_dev = sp_count // PLANES * tp_count
    dc = width // chunks
    ff = w_gate.shape[1]
    vm = pl.BlockSpec(memory_space=pltpu.VMEM)
    hb = pl.BlockSpec(memory_space=pl.ANY)
    slots = n_dev * cap
    blocks = pltpu.VMEM((PLANES, chunks, n_dev, cap, dc), BF)
    table = pltpu.VMEM((PLANES, slots, rows), BF)
    dma = pltpu.SemaphoreType.DMA
    return pl.pallas_call(
        functools.partial(layer_kernel, sp_count, tp_count, cap, chunks),
        out_shape=jax.ShapeDtypeStruct((rows, width), BF),
        in_specs=[vm] * 8 + [hb] * 4,
        out_specs=vm,
        scratch_shapes=[
            pltpu.VMEM((width, ff), BF),
            pltpu.VMEM((width, ff), BF),
            pltpu.VMEM((ff, width), BF),
            pltpu.VMEM((PLANES, chunks, rows, dc), BF),
            pltpu.VMEM((PLANES, 8, rows), F32),
            blocks,
            blocks,
            pltpu.VMEM((PLANES, slots, ff), BF),
            pltpu.VMEM((slots, ff), F32),
            pltpu.VMEM((slots, ff), F32),
            blocks,
            blocks,
            pltpu.VMEM((3, chunks, rows, dc), F32),
            pltpu.VMEM((3, chunks, rows, dc), BF),
            pltpu.VMEM((5, chunks, rows, dc), BF),
            pltpu.VMEM((rows, width), F32),
            table,
            pltpu.VMEM((PLANES, rows, 2 * slots), BF),
            pltpu.VMEM(ow.shape, BF),
            pltpu.VMEM((length + 2 * halo, local_width), BF),
            pltpu.VMEM((length + 2 * halo, local_width), F32),
            pltpu.VMEM((2, rows // 2, local_width), F32),
            pltpu.VMEM((2, rows, local_width), F32),
            pltpu.VMEM(gain.shape, F32),
            dma((4,)),
            dma((PLANES,)),
            dma((PLANES,)),
            dma((5, chunks)),
            dma((PLANES, chunks)),
            dma((PLANES, chunks)),
            dma((PLANES, chunks)),
            dma((PLANES, chunks)),
            dma((PLANES, chunks)),
            dma((3, chunks)),
            dma((5, chunks)),
            dma((4,)),
            dma((2, 2)),
            dma((2,)),
        ],
        compiler_params=pltpu.CompilerParams(
            collective_id=0, has_side_effects=True, vmem_limit_bytes=58 * 1024 * 1024
        ),
        name="layer",
    )(resid, value_in, gate_in, taps_w, gain, ffn_gain, ids, mix, ow, w_gate, w_up, w_down)


def per_device(
    resid,
    value_in,
    gate_in,
    conv_weight,
    norm_gain,
    out_weight,
    ffn_gain,
    expert_ids,
    expert_mix,
    w_gate,
    w_up,
    w_down,
):
    experts_all = lax.axis_size("sp") * lax.axis_size("tp")
    rows_here = resid.shape[0]
    topk = expert_ids.shape[1]
    cap = max(2, (2 * topk * rows_here + experts_all - 1) // experts_all)
    return layer_call(
        resid, value_in, gate_in, conv_weight, norm_gain, ffn_gain[None], expert_ids.T, expert_mix.T,
        out_weight, w_gate[0], w_up[0], w_down[0], cap,
    )


def solution(mesh):
    return jax.shard_map(
        per_device,
        mesh=mesh,
        in_specs=(
            P(("sp", "tp"), None),
            P("sp", "tp"),
            P("sp", "tp"),
            P(None, "tp"),
            P("tp"),
            P(),
            P(),
            P(("sp", "tp"), None),
            P(("sp", "tp"), None),
            P(("sp", "tp"), None, None),
            P(("sp", "tp"), None, None),
            P(("sp", "tp"), None, None),
        ),
        out_specs=P(("sp", "tp"), None),
        check_vma=False,
    )
```

```python
import functools
import jax
import jax.numpy as jnp
from jax import lax
from jax.experimental import pallas as pl
from jax.experimental.pallas import tpu as pltpu
from jax.sharding import PartitionSpec as P

MESH = pl.DeviceIdType.MESH
BF = jnp.bfloat16
F32 = jnp.float32


PLANES = 4


def layer_kernel(
    sp_count, tp_count, cap, chunks,
    resid, value_in, gate_in, taps_w, gain, ffn_gain, ids, mix, ow_h, wg_h, wu_h, wd_h, out,
    wg, wu, wd, tok, infos, pack, rx, hid, gates, ups, ys, yr, part, sums, back, acc,
    hots, mixes, ow, gp, wide_in, cs, cf, gf,
    w_sem, i_send, i_recv, t_send, t_recv, d_send, d_recv, r_send, r_recv, b_send, b_recv,
    h_sem, c_sem, g_sem,
):
    plane = sp_count // PLANES
    n_dev = plane * tp_count
    rows, width = resid.shape
    dc = width // chunks
    slots = n_dev * cap
    me_sp = lax.axis_index("sp")
    me_tp = lax.axis_index("tp")
    local = lax.rem(me_sp, plane)
    base = me_sp - local
    mine = local * tp_count + me_tp
    level = me_sp // plane
    low_half = level < PLANES // 2
    step_in = jnp.where(low_half, plane, -plane)
    is_end = (level == 0) | (level == PLANES - 1)
    is_mid = jnp.logical_not(is_end)
    inner = (me_sp + step_in, me_tp)
    outer = (jnp.where(is_mid, me_sp - step_in, me_sp), me_tp)

    def column(i):
        return (lax.rem(me_sp + i * plane, sp_count), me_tp)

    def peer(i):
        n = lax.rem(mine + i, n_dev)
        return n, (base + n // tp_count, lax.rem(n, tp_count))

    weights = [
        pltpu.make_async_copy(h, v, w_sem.at[k])
        for k, (h, v) in enumerate(((ow_h, ow), (wg_h, wg), (wu_h, wu), (wd_h, wd)))
    ]
    for w in weights:
        w.start()

    barrier = pltpu.get_barrier_semaphore()

    @pl.loop(1, n_dev)
    def _(i):
        pl.semaphore_signal(barrier, inc=1, device_id=peer(i)[1], device_id_type=MESH)

    @pl.loop(1, PLANES)
    def _(i):
        pl.semaphore_signal(barrier, inc=1, device_id=column(i), device_id_type=MESH)

    last = sp_count - 1
    has_low, has_high = me_sp > 0, me_sp < last
    lower = (jnp.maximum(me_sp - 1, 0), me_tp)
    upper = (jnp.minimum(me_sp + 1, last), me_tp)
    twin = (me_sp, 1 - me_tp)

    @pl.when(has_low)
    def _():
        pl.semaphore_signal(barrier, inc=1, device_id=lower, device_id_type=MESH)

    @pl.when(has_high)
    def _():
        pl.semaphore_signal(barrier, inc=1, device_id=upper, device_id_type=MESH)

    length, local_width = value_in.shape
    taps = taps_w.shape[0]
    reach = taps // 2
    halo = (reach + 15) // 16 * 16
    half = rows // 2
    span = half + 2 * halo
    gated = (value_in[...].astype(F32) * jax.nn.sigmoid(gate_in[...].astype(F32))).astype(BF)
    gp[halo : halo + length, :] = gated
    wide_in[halo : halo + length, :] = gated.astype(F32)

    @pl.when(jnp.logical_not(has_low))
    def _():
        gp[0:halo, :] = jnp.zeros((halo, local_width), BF)

    @pl.when(jnp.logical_not(has_high))
    def _():
        gp[halo + length :, :] = jnp.zeros((halo, local_width), BF)

    def begins(h, core):
        return pl.multiple_of(half + half * core if h == 0 else (length - half) * core, half)

    def inside(h, core):
        return pl.ds(pl.multiple_of(half * (1 - core) if h == 0 else half * core, half), half)

    def convolve(h, core, put):
        first = begins(h, core)

        @pl.loop(0, local_width // 128)
        def _(b):
            cols = pl.ds(pl.multiple_of(b * 128, 128), 128)
            x = wide_in[pl.ds(first, span), cols]
            total = jnp.zeros((half, 128), F32)
            for r in range(8):
                offsets = [j for j in range(taps) if (j + halo - reach) % 8 == r]
                if not offsets:
                    continue
                shifted = x if r == 0 else pltpu.roll(x, span - r, 0)
                for j in offsets:
                    at = j + halo - reach - r
                    total = total + shifted[at : at + half] * taps_w[j : j + 1, cols]
            put(cols, total)

    def both(h):
        def put_out(cols, total):
            cs[h, :, cols] = total

        def put_own(cols, total):
            cf[0, inside(h, me_tp), cols] = total

        return put_out, put_own

    convolve(0, 1 - me_tp, both(0)[0])
    convolve(0, me_tp, both(0)[1])

    pl.semaphore_wait(
        barrier,
        n_dev - 1 + PLANES - 1 + has_low.astype(jnp.int32) + has_high.astype(jnp.int32),
    )

    def remote(src, dst, send, recv, where):
        return pltpu.make_async_remote_copy(
            src_ref=src, dst_ref=dst, send_sem=send, recv_sem=recv,
            device_id=where, device_id_type=MESH,
        )

    to_low = remote(
        gp.at[halo : 2 * halo], gp.at[halo + length : 2 * halo + length], h_sem.at[0], h_sem.at[1], lower
    )
    to_high = remote(gp.at[length : length + halo], gp.at[0:halo], h_sem.at[2], h_sem.at[3], upper)

    @pl.when(has_low)
    def _():
        to_low.start()

    @pl.when(has_high)
    def _():
        to_high.start()

    def conv_copy(h):
        there = inside(h, 1 - me_tp)
        return remote(cs.at[h], cf.at[1, there], c_sem.at[0, h], c_sem.at[1, h], twin)

    conv_copy(0).start()
    gain_copy = remote(gain, gf, g_sem.at[0], g_sem.at[1], twin)
    gain_copy.start()

    experts_all = sp_count * tp_count
    expert = lax.broadcasted_iota(jnp.int32, (experts_all, rows), 0).astype(F32)
    named = ids[...].astype(F32)
    hot = [jnp.where(expert == named[k : k + 1, :], 1.0, 0.0) for k in range(2)]
    earlier = lax.broadcasted_iota(jnp.int32, (rows, rows), 0)
    later = lax.broadcasted_iota(jnp.int32, (rows, rows), 1)
    before = jnp.where(earlier < later, 1.0, 0.0).astype(BF)
    rank = jnp.dot((hot[0] + hot[1]).astype(BF), before, preferred_element_type=F32)
    infos[0, 2:4, :] = mix[...]
    infos[0, 4:, :] = jnp.zeros((4, rows), F32)
    for k in range(2):
        infos[0, k : k + 1, :] = named[k : k + 1, :] * cap + jnp.sum(
            hot[k] * rank, axis=0, keepdims=True
        )

    def place(there):
        at_end = (there == 0) | (there == PLANES - 1)
        gap = jnp.abs(there - level)
        return jnp.where(at_end, gap, jnp.where(is_end, jnp.where(gap == 1, 1, 3), 2))

    info_copies = []
    for i in range(1, PLANES):
        there = lax.rem(level + i, PLANES)
        info_copies.append(
            remote(infos.at[0], infos.at[place(there)], i_send.at[i], i_recv.at[place(there)], column(i))
        )
    for copy in info_copies:
        copy.start()

    channels = local_width * tp_count
    whose = (me_tp, 1 - me_tp)
    step = 512

    def silu(v):
        return v * jax.nn.sigmoid(v)

    def hop(q, src, k, c, where):
        return remote(tok.at[src, c], tok.at[k, c], t_send.at[q, c], t_recv.at[k, c], where)

    def hop_part(q, k, c, where, at):
        return remote(tok.at[0, c, at], tok.at[k, c, at], t_send.at[q, c], t_recv.at[k, c], where)

    def tokens(h):
        here = inside(h, me_tp)
        remote(cs.at[h], cf.at[1, here], c_sem.at[0, h], c_sem.at[1, h], twin).wait_recv()
        conv = [cf[i, here, :] for i in range(2)]
        mean = sum(jnp.sum(v, axis=1, keepdims=True) for v in conv) / channels
        msq = sum(jnp.sum(v * v, axis=1, keepdims=True) for v in conv) / channels
        scale = lax.rsqrt(msq - mean * mean + 1e-05)
        mixed = [
            silu((v - mean) * scale * g[...].reshape(1, local_width)).astype(BF)
            for v, g in zip(conv, (gain, gf))
        ]
        square = jnp.zeros((half, 1), F32)
        for c in range(width // step):
            cols = slice(c * step, (c + 1) * step)
            proj = jnp.zeros((half, step), F32)
            for m, w in zip(mixed, whose):
                at = pl.ds(pl.multiple_of(w * local_width, local_width), local_width)
                proj = proj + jnp.dot(m, ow[at, cols], preferred_element_type=F32)
            wide = (resid[here, cols].astype(F32) + proj).astype(BF).astype(F32)
            acc[here, cols] = wide
            square = square + jnp.sum(wide * wide, axis=1, keepdims=True)
        rms = lax.rsqrt(square / width + 1e-06)
        for c in range(chunks):
            at = slice(c * dc, (c + 1) * dc)
            tok[0, c, here, :] = (acc[here, at] * rms * ffn_gain[:, at]).astype(BF)

            @pl.when(is_mid)
            def _():
                hop_part(0, 2, c, inner, here).start()
                hop_part(1, 1, c, outer, here).start()

            @pl.when(is_end)
            def _():
                hop_part(0, 1, c, inner, here).start()

    weights[0].wait()
    gain_copy.wait_recv()
    tokens(0)

    @pl.when(has_low)
    def _():
        to_high.wait_recv()

    @pl.when(has_high)
    def _():
        to_low.wait_recv()

    wide_in[0:halo, :] = gp[0:halo, :].astype(F32)
    wide_in[halo + length :, :] = gp[halo + length :, :].astype(F32)
    convolve(1, 1 - me_tp, both(1)[0])
    conv_copy(1).start()
    convolve(1, me_tp, both(1)[1])
    tokens(1)

    def slot_match(ref):
        ids = lax.broadcasted_iota(jnp.int32, (slots, rows), 0) + base * (tp_count * cap)
        ids = ids.astype(F32)
        return ids == ref[0:1, :], ids == ref[1:2, :]

    def tables(k):
        a, b = slot_match(infos.at[k])
        hots[k] = jnp.where(a | b, 1.0, 0.0).astype(BF)
        full = jnp.where(a, infos[k, 2:3, :], 0.0) + jnp.where(b, infos[k, 3:4, :], 0.0)
        full = jnp.transpose(full)
        high = full.astype(BF)
        mixes[k, :, :slots] = high
        mixes[k, :, slots:] = (full - high.astype(F32)).astype(BF)

    few = n_dev <= 8
    peers = [peer(i) for i in range(1, n_dev)] if few else []

    def exchange(src, dst, send, recv, k, c):
        def start(n, where):
            remote(src.at[k, c, n], dst.at[k, c, mine], send.at[k, c], recv.at[k, c], where).start()

        if few:
            for n, where in peers:
                start(n, where)
        else:

            @pl.loop(1, n_dev)
            def _(i):
                start(*peer(i))

        dst[k, c, mine] = src[k, c, mine]

    def all_in(dst, recv, k, c):
        share = dst.at[k, c, pl.ds(0, n_dev - 1)]
        pltpu.make_async_copy(share, share, recv.at[k, c]).wait()

    def all_out(src, send, k, c):
        share = src.at[k, c, pl.ds(0, n_dev - 1)]
        pltpu.make_async_copy(share, share, send.at[k, c]).wait()

    def dispatch(k, c):
        picked = jnp.dot(hots[k], tok[k, c], preferred_element_type=F32)
        pack[k, c] = picked.astype(BF).reshape(n_dev, cap, dc)
        exchange(pack, rx, d_send, d_recv, k, c)

    def arrived(k, c):
        hop(0, k, k, c, inner).wait_recv()

    ff = wg.shape[1]
    tile = min(256, ff)
    pairs = chunks // 2

    def hidden(*ks):
        for k in ks:
            for c in range(chunks):
                all_in(rx, d_recv, k, c)
        n = len(ks) * slots

        @pl.loop(0, ff // tile)
        def _(f):
            cols = pl.ds(pl.multiple_of(f * tile, tile), tile)
            gate = jnp.zeros((n, tile), F32)
            up = jnp.zeros((n, tile), F32)
            for c in range(chunks):
                x = [rx[k, c].reshape(slots, dc) for k in ks]
                x = x[0] if len(ks) == 1 else jnp.concatenate(x, axis=0)
                at = slice(c * dc, (c + 1) * dc)
                gate = gate + jnp.dot(x, wg[at, cols], preferred_element_type=F32)
                up = up + jnp.dot(x, wu[at, cols], preferred_element_type=F32)
            made = (gate * jax.nn.sigmoid(gate) * up).astype(BF)
            for i, k in enumerate(ks):
                hid[k, :, cols] = made[i * slots : (i + 1) * slots]

    def hidden_part(k, j):
        for c in (2 * j, 2 * j + 1):
            all_in(rx, d_recv, k, c)

        @pl.loop(0, ff // tile)
        def _(f):
            cols = pl.ds(pl.multiple_of(f * tile, tile), tile)
            gate = up = None
            for c in (2 * j, 2 * j + 1):
                x = rx[k, c].reshape(slots, dc)
                at = slice(c * dc, (c + 1) * dc)
                g = jnp.dot(x, wg[at, cols], preferred_element_type=F32)
                u = jnp.dot(x, wu[at, cols], preferred_element_type=F32)
                gate, up = (g, u) if gate is None else (gate + g, up + u)
            if j > 0:
                gate, up = gate + gates[:, cols], up + ups[:, cols]
            if j < pairs - 1:
                gates[:, cols] = gate
                ups[:, cols] = up
            else:
                hid[k, :, cols] = (gate * jax.nn.sigmoid(gate) * up).astype(BF)

    def answer(k, c):
        exchange(ys, yr, r_send, r_recv, k, c)

    def reply(k, *cs):
        for c in cs:
            answer(k, c)

    def down(ks, cs, send=()):
        for c in cs:
            x = [hid[k] for k in ks]
            x = x[0] if len(ks) == 1 else jnp.concatenate(x, axis=0)
            y = jnp.dot(x, wd[:, c * dc : (c + 1) * dc], preferred_element_type=F32).astype(BF)
            for i, k in enumerate(ks):
                ys[k, c] = y[i * slots : (i + 1) * slots].reshape(n_dev, cap, dc)
                if k in send:
                    answer(k, c)

    def combine(k, c):
        all_in(yr, r_recv, k, c)
        y = yr[k, c].reshape(slots, dc)
        return jnp.dot(mixes[k], jnp.concatenate([y, y], axis=0), preferred_element_type=F32)

    def homeward(q, slot, c, where):
        return remote(sums.at[q, c], back.at[slot, c], b_send.at[q, c], b_recv.at[slot, c], where)

    def returned(slot, c):
        homeward(0, slot, c, inner).wait_recv()
        return back[slot, c].astype(F32)

    def send_home(q, slot, c, where, value):
        sums[q, c] = value.astype(BF)
        homeward(q, slot, c, where).start()

    def add(c, value):
        acc[:, c * dc : (c + 1) * dc] += value

    tables(0)
    for c in range(chunks):
        dispatch(0, c)
    for k in range(1, PLANES):
        remote(infos.at[0], infos.at[k], i_send.at[k], i_recv.at[k], inner).wait_recv()
        tables(k)

    def take(k, *cs):
        for c in cs:
            arrived(k, c)
            dispatch(k, c)

    for w in weights[1:]:
        w.wait()
    every = range(chunks)

    @pl.when(is_end)
    def _():
        def own(*cs):
            for c in cs:
                add(c, combine(0, c))

        def out_of(*cs):
            for c in cs:
                at = slice(c * dc, (c + 1) * dc)
                out[:, at] = (acc[:, at] + returned(0, c)).astype(BF)

        def home(k, *cs):
            for c in cs:
                send_home(k - 1, k - 1, c, inner, combine(k, c))

        take(1, 2, 0, 1)
        hidden(0)
        take(1, 4)
        down((0,), (4,))
        reply(0, 4)
        take(1, 5, 6)
        down((0,), (0,))
        take(1, 7, 3)
        take(2, 1, 0, 2, 4)
        hidden(1)
        down((1,), (1,), send=(1,))
        take(2, 3)
        down((1,), (0,), send=(1,))
        take(2, 6, 5, 7)
        down((1,), (4,), send=(1,))
        down((0,), (7,))
        take(3, 2)
        home(1, 1, 0)
        down((1,), (3, 7), send=(1,))
        take(3, 3)
        hidden(2)
        take(3, 0)
        down((0,), (5,))
        down((2,), (0,), send=(2,))
        home(1, 3)
        take(3, 1)
        down((0,), (2,))
        down((2,), (1,), send=(2,))
        home(1, 4)
        down((2,), (6,), send=(2,))
        take(3, 4)
        down((2,), (4,), send=(2,))
        home(1, 7)
        take(3, 7, 5)
        home(2, 0)
        hidden_part(3, 0)
        take(3, 6)
        down((2,), (3,), send=(2,))
        home(2, 1)
        reply(0, 2)
        home(2, 6)
        down((2,), (2,), send=(2,))
        home(2, 4)
        hidden_part(3, 1)
        hidden_part(3, 2)
        reply(0, 0)
        hidden_part(3, 3)
        down((3,), (2,), send=(3,))
        home(2, 3)
        down((3,), (7, 4), send=(3,))
        down((2,), (5,), send=(2,))
        down((3,), (5,), send=(3,))
        home(2, 2)
        down((3,), (1,), send=(3,))
        own(4)
        reply(0, 7)
        down((3,), (6,), send=(3,))
        home(3, 2)
        down((3,), (0,), send=(3,))
        home(3, 7)
        own(2)
        home(3, 4)
        down((3,), (3,), send=(3,))
        down((1,), (6,), send=(1,))
        home(3, 1)
        down((1,), (2,), send=(1,))
        down((0,), (6,))
        down((2,), (7,), send=(2,))
        own(7)
        home(3, 5, 3, 6, 0)
        down((0,), (1, 3))
        reply(0, 5)
        home(1, 6)
        reply(0, 3)
        home(1, 2)
        reply(0, 1)
        down((1,), (5,), send=(1,))
        reply(0, 6)
        home(2, 5, 7)
        own(1)
        out_of(1)
        own(6)
        out_of(2)
        home(1, 5)
        own(3)
        out_of(3, 4, 6)
        own(0, 5)
        out_of(5, 7, 0)
        for c in range(chunks):
            hop(0, 0, 1, c, inner).wait_send()

    @pl.when(is_mid)
    def _():
        def near(*cs):
            for c in cs:
                arrived(1, c)
                hop(2, 1, 3, c, inner).start()
                dispatch(1, c)
                arrived(2, c)
                hop(3, 2, 2, c, outer).start()
                dispatch(2, c)

        def far(*cs):
            for c in cs:
                arrived(3, c)
                hop(4, 3, 3, c, outer).start()
                dispatch(3, c)

        def keep(k, *cs):
            for c in cs:
                part[k - 1, c] = combine(k, c)

        def pass_on(q, k, slot, got, where, c):
            send_home(q, slot, c, where, part[k - 1, c] + returned(got, c))

        def finish(*cs):
            for c in cs:
                at = slice(c * dc, (c + 1) * dc)
                value = combine(0, c) + returned(0, c) + returned(3, c)
                out[:, at] = (acc[:, at] + value).astype(BF)

        def middle(*cs):
            for c in cs:
                pass_on(0, 2, 3, 1, inner, c)

        def onward(*cs):
            for c in cs:
                pass_on(1, 3, 4, 2, inner, c)

        def late(*cs):
            for c in cs:
                pass_on(2, 1, 0, 4, outer, c)

        near(4, 0, 1, 2, 3)
        hidden(0)
        near(5)
        down((0,), (7, 1))
        near(6, 7)
        far(2, 3, 0)
        hidden(1, 2)
        down((1, 2), (7,), send=(1,))
        far(1)
        reply(0, 7)
        far(4)
        down((0,), (6,))
        down((1, 2), (5,), send=(1,))
        reply(2, 7)
        down((0,), (3,))
        down((1, 2), (4, 0), send=(1,))
        far(7, 5, 6)
        down((0,), (2,))
        reply(2, 0)
        down((1, 2), (3, 1), send=(1,))
        down((0,), (0,))
        down((1, 2), (6,), send=(1,))
        reply(2, 4)
        reply(0, 3)
        keep(1, 7)
        hidden(3)
        down((1, 2), (2,), send=(1,))
        keep(2, 0)
        reply(0, 0)
        down((3,), (2,), send=(3,))
        reply(2, 6)
        down((3,), (5,), send=(3,))
        down((0,), (5,))
        down((3,), (1,), send=(3,))
        reply(2, 1, 2)
        down((3,), (0,), send=(3,))
        keep(1, 2)
        middle(0)
        down((3,), (4,), send=(3,))
        keep(2, 6, 4)
        middle(6)
        down((3,), (3, 7), send=(3,))
        keep(1, 5)
        down((3,), (6,), send=(3,))
        reply(2, 5)
        middle(4)
        keep(2, 1)
        middle(1)
        reply(0, 6)
        keep(1, 1)
        keep(3, 1, 0)
        keep(1, 4)
        reply(2, 3)
        keep(3, 4)
        keep(1, 3)
        keep(3, 2)
        onward(2)
        keep(3, 7)
        onward(7)
        keep(1, 6)
        onward(4, 1)
        keep(3, 5)
        late(2)
        keep(2, 7)
        keep(3, 6, 3)
        keep(2, 3)
        onward(5)
        late(7)
        down((0,), (4,))
        onward(3)
        reply(0, 4)
        late(4)
        onward(6)
        keep(1, 0)
        late(1)
        onward(0)
        reply(0, 1)
        late(5)
        reply(0, 2)
        keep(2, 2)
        middle(3)
        late(3)
        reply(0, 5)
        keep(2, 5)
        middle(2)
        late(6)
        finish(6)
        middle(5)
        late(0)
        middle(7)
        finish(4, 2, 1, 0, 3, 5, 7)
        for c in range(chunks):
            hop(0, 0, 2, c, inner).wait_send()
            hop(1, 0, 1, c, outer).wait_send()
            hop(2, 1, 3, c, inner).wait_send()
            hop(3, 2, 2, c, outer).wait_send()
            hop(4, 3, 3, c, outer).wait_send()

    for copy in info_copies:
        copy.wait_send()
    gain_copy.wait_send()
    conv_copy(0).wait_send()
    conv_copy(1).wait_send()

    @pl.when(has_low)
    def _():
        to_low.wait_send()

    @pl.when(has_high)
    def _():
        to_high.wait_send()

    for c in range(chunks):
        for q in range(3):
            homeward(q, q, c, inner).wait_send()
        for k in range(PLANES):
            all_out(pack, d_send, k, c)
            all_out(ys, r_send, k, c)


def layer_call(resid, value_in, gate_in, taps_w, gain, ffn_gain, ids, mix, ow, w_gate, w_up, w_down, cap):
    sp_count, tp_count = lax.axis_size("sp"), lax.axis_size("tp")
    chunks = 8
    rows, width = resid.shape
    length, local_width = value_in.shape
    halo = (taps_w.shape[0] // 2 + 15) // 16 * 16
    n_dev = sp_count // PLANES * tp_count
    dc = width // chunks
    ff = w_gate.shape[1]
    vm = pl.BlockSpec(memory_space=pltpu.VMEM)
    hb = pl.BlockSpec(memory_space=pl.ANY)
    slots = n_dev * cap
    blocks = pltpu.VMEM((PLANES, chunks, n_dev, cap, dc), BF)
    table = pltpu.VMEM((PLANES, slots, rows), BF)
    dma = pltpu.SemaphoreType.DMA
    return pl.pallas_call(
        functools.partial(layer_kernel, sp_count, tp_count, cap, chunks),
        out_shape=jax.ShapeDtypeStruct((rows, width), BF),
        in_specs=[vm] * 8 + [hb] * 4,
        out_specs=vm,
        scratch_shapes=[
            pltpu.VMEM((width, ff), BF),
            pltpu.VMEM((width, ff), BF),
            pltpu.VMEM((ff, width), BF),
            pltpu.VMEM((PLANES, chunks, rows, dc), BF),
            pltpu.VMEM((PLANES, 8, rows), F32),
            blocks,
            blocks,
            pltpu.VMEM((PLANES, slots, ff), BF),
            pltpu.VMEM((slots, ff), F32),
            pltpu.VMEM((slots, ff), F32),
            blocks,
            blocks,
            pltpu.VMEM((3, chunks, rows, dc), F32),
            pltpu.VMEM((3, chunks, rows, dc), BF),
            pltpu.VMEM((5, chunks, rows, dc), BF),
            pltpu.VMEM((rows, width), F32),
            table,
            pltpu.VMEM((PLANES, rows, 2 * slots), BF),
            pltpu.VMEM(ow.shape, BF),
            pltpu.VMEM((length + 2 * halo, local_width), BF),
            pltpu.VMEM((length + 2 * halo, local_width), F32),
            pltpu.VMEM((2, rows // 2, local_width), F32),
            pltpu.VMEM((2, rows, local_width), F32),
            pltpu.VMEM(gain.shape, F32),
            dma((4,)),
            dma((PLANES,)),
            dma((PLANES,)),
            dma((5, chunks)),
            dma((PLANES, chunks)),
            dma((PLANES, chunks)),
            dma((PLANES, chunks)),
            dma((PLANES, chunks)),
            dma((PLANES, chunks)),
            dma((3, chunks)),
            dma((5, chunks)),
            dma((4,)),
            dma((2, 2)),
            dma((2,)),
        ],
        compiler_params=pltpu.CompilerParams(
            collective_id=0, has_side_effects=True, vmem_limit_bytes=58 * 1024 * 1024
        ),
        name="layer",
    )(resid, value_in, gate_in, taps_w, gain, ffn_gain, ids, mix, ow, w_gate, w_up, w_down)


def per_device(
    resid,
    value_in,
    gate_in,
    conv_weight,
    norm_gain,
    out_weight,
    ffn_gain,
    expert_ids,
    expert_mix,
    w_gate,
    w_up,
    w_down,
):
    experts_all = lax.axis_size("sp") * lax.axis_size("tp")
    rows_here = resid.shape[0]
    topk = expert_ids.shape[1]
    cap = max(2, (2 * topk * rows_here + experts_all - 1) // experts_all)
    return layer_call(
        resid, value_in, gate_in, conv_weight, norm_gain, ffn_gain[None], expert_ids.T, expert_mix.T,
        out_weight, w_gate[0], w_up[0], w_down[0], cap,
    )


def solution(mesh):
    return jax.shard_map(
        per_device,
        mesh=mesh,
        in_specs=(
            P(("sp", "tp"), None),
            P("sp", "tp"),
            P("sp", "tp"),
            P(None, "tp"),
            P("tp"),
            P(),
            P(),
            P(("sp", "tp"), None),
            P(("sp", "tp"), None),
            P(("sp", "tp"), None, None),
            P(("sp", "tp"), None, None),
            P(("sp", "tp"), None, None),
        ),
        out_specs=P(("sp", "tp"), None),
        check_vma=False,
    )
```
